512 devices in a mesh: sp: 32 (over z, core), tp: 16 (over y, x).
Axes of the slice: x: 4, y: 4, z: 16, core: 2. Of those that a mesh axis runs over, the one named last changes fastest.
Arguments:
- query_a: bfloat16 [1024, 4096], P('tp', 'sp'), may hold values from -16 to 16
- key_a: bfloat16 [1024, 4096], P('tp', 'sp'), may hold values from -6 to 6
- value_a: bfloat16 [1024, 4096], P('tp', 'sp'), may hold values from -6 to 6
- cumlog_a: float32 [16, 4096], P('tp'), as said below
- query_b: bfloat16 [2048, 4096], P('tp', 'sp'), may hold values from -16 to 16
- key_b: bfloat16 [2048, 4096], P('tp', 'sp'), may hold values from -6 to 6
- value_b: bfloat16 [2048, 4096], P('tp', 'sp'), may hold values from -6 to 6
- cumlog_b: float32 [16, 4096], P('tp'), as said below
- out_weight_a: bfloat16 [1024, 2048], P('tp'), may hold values from -0.375 to 0.375
- out_weight_b: bfloat16 [2048, 2048], P('tp'), may hold values from -0.25 to 0.25
- residual: bfloat16 [4096, 2048], P(('sp', 'tp')), may hold values from -6 to 6
- norm_gain: float32 [2048], replicated, may hold values from 0.1 to 1.9
- expert_ids: int32 [4096, 2], P('sp'), may hold values from 0 to 31, as said below
- route_weight: float32 [4096, 2], P('sp'), may hold values from 0.1 to 1
- gate_w: bfloat16 [32, 2048, 1024], P('sp', None, 'tp'), may hold values from -0.125 to 0.125
- up_w: bfloat16 [32, 2048, 1024], P('sp', None, 'tp'), may hold values from -0.125 to 0.125
- down_w: bfloat16 [32, 1024, 2048], P('sp', None, 'tp'), may hold values from -0.1875 to 0.1875
Outputs:
- layer_out: bfloat16 [4096, 2048], P('sp', 'tp')
The draws below stay inside these ranges and needn't reach their ends.
Inputs may be any that keep to these rules, and one draw needn't show every extreme that they name: `expert_ids`: each row names two different experts of one group (expert e is in group e // 8). In every aligned block of 128 rows (one index of sp) no expert is named more than 16 times, and every expert of one group, the same group for all blocks, is named exactly 16 times. `cumlog_a`: along positions the values of each head never increase. `cumlog_b`: along positions the values of each head never increase.
All inputs are finite; a program needn't handle non-finite values.
Results may differ from the reference program's by a relative error of at most 0.017.
Values may be sent and summed in bfloat16 or wider, within the bound.
A program may use at most 64 MiB of HBM per device.

```python
import jax
import jax.numpy as jnp
from jax import lax

D = 2048
HA = 16
HDA = 64
HB = 16
HDB = 128
DFF = 1024
GROUPS = 4
TOP = 2
TOK_DEV = 128
TOKENS = 4096
EXPERTS = 32
GSZ = 8
CAP = 16
N_SP = 32
N_TP = 16


def query_like(key, rows, salt):
    own = jax.random.fold_in(key, salt)
    base = jnp.clip(2.5 * jax.random.normal(own, (rows, TOKENS), jnp.float32), -15.0, 15.0)
    return base.astype(jnp.bfloat16)


def key_like(key, rows, salt):
    own = jax.random.fold_in(key, salt)
    base = jnp.clip(jax.random.normal(own, (rows, TOKENS), jnp.float32), -6.0, 6.0)
    return base.astype(jnp.bfloat16)


def draw_query_a(key, part):
    return query_like(key, HA * HDA, 1)


def draw_key_a(key, part):
    return key_like(key, HA * HDA, 2)


def draw_query_b(key, part):
    return query_like(key, HB * HDB, 3)


def draw_key_b(key, part):
    return key_like(key, HB * HDB, 4)


def gate_totals(key, heads):
    order = jax.random.permutation(jax.random.fold_in(key, 11), heads)
    slow = order < heads // 2
    rate_slow = 1.5 / TOKENS * jax.random.uniform(jax.random.fold_in(key, 12), (heads,), jnp.float32, 0.5, 1.2)
    rate_fast = jax.random.uniform(jax.random.fold_in(key, 13), (heads,), jnp.float32, 0.01, 0.033)
    rate = jnp.where(slow, rate_slow, rate_fast)
    block_factor = jnp.exp(jax.random.uniform(jax.random.fold_in(key, 14), (heads, TOKENS // TOK_DEV), jnp.float32, -0.9, 0.9))
    factor = jnp.repeat(block_factor, TOK_DEV, axis=1)
    rough = jax.random.uniform(jax.random.fold_in(key, 15), (heads, TOKENS), jnp.float32, 0.3, 1.7)
    return jnp.cumsum(-rate[:, None] * factor * rough, axis=1).astype(jnp.float32)


def draw_cumlog_a(key, part):
    return gate_totals(jax.random.fold_in(key, 5), HA)


def draw_cumlog_b(key, part):
    return gate_totals(jax.random.fold_in(key, 6), HB)


def draw_expert_ids(key, part):
    hot = jax.random.randint(jax.random.fold_in(key, 21), (), 0, GROUPS)

    def one_block(block_index):
        block_key = jax.random.fold_in(key, 1000 + block_index)

        def group_pairs(group):
            perm = jax.random.permutation(jax.random.fold_in(block_key, group), GSZ)
            spots = jnp.arange(TOK_DEV // 2) % GSZ
            return jnp.stack([perm[spots], perm[(spots + 1) % GSZ]], axis=-1) + group * GSZ
        pairs = jax.vmap(group_pairs)(jnp.arange(GROUPS))
        order = jnp.argsort(jnp.where(jnp.arange(GROUPS) == hot, 0, 1), stable=True)
        pairs = pairs[order]
        others = pairs[1:].reshape(-1, 2)
        chosen = jax.random.permutation(jax.random.fold_in(block_key, 50), others.shape[0])[:TOK_DEV // 2]
        rows = jnp.concatenate([pairs[0], others[chosen]], axis=0)
        shuffle = jax.random.permutation(jax.random.fold_in(block_key, 51), TOK_DEV)
        return rows[shuffle]
    blocks = jax.vmap(one_block)(jnp.arange(TOKENS // TOK_DEV))
    return blocks.reshape(TOKENS, TOP).astype(jnp.int32)


def level_of(key, extent, cuts, smallest, high):
    def one(position, blocks):
        steps = jax.random.uniform(jax.random.fold_in(jax.random.fold_in(key, 6), position), (blocks,), jnp.float32, smallest / len(cuts), high / len(cuts))
        return jnp.repeat(jnp.exp(steps), extent[position] // blocks).reshape((-1,) + (1,) * (len(extent) - position - 1))

    loudness = one(*cuts[0])
    for cut in cuts[1:]:
        loudness = loudness * one(*cut)
    return loudness


def gaussian(own_key, dims, deviation, limit, split=(), kind=jnp.bfloat16):
    array = deviation * jax.random.normal(own_key, dims, jnp.float32)
    if split:
        array = array * level_of(own_key, dims, split, -0.22, 0.18)
    return jnp.clip(array, -limit, limit).astype(kind)


def setup_inputs(seed: int = 0) -> dict:
    key_list = jax.random.split(jax.random.key(seed), 18)
    query_a = draw_query_a(jax.random.fold_in(key_list[17], 71), 0)
    key_a = draw_key_a(jax.random.fold_in(key_list[17], 71), 0)
    value_a = gaussian(key_list[2], (HA * HDA, TOKENS), 1.0, 6.0, ((0, 16), (1, 32)))
    cumlog_a = draw_cumlog_a(jax.random.fold_in(key_list[17], 71), 0)
    query_b = draw_query_b(jax.random.fold_in(key_list[17], 71), 0)
    key_b = draw_key_b(jax.random.fold_in(key_list[17], 71), 0)
    value_b = gaussian(key_list[6], (HB * HDB, TOKENS), 1.0, 6.0, ((0, 16), (1, 32)))
    cumlog_b = draw_cumlog_b(jax.random.fold_in(key_list[17], 71), 0)
    out_weight_a = gaussian(key_list[8], (HA * HDA, D), (HA * HDA // 4) ** -0.5, 0.375, ((0, 16),))
    out_weight_b = gaussian(key_list[9], (HB * HDB, D), (HB * HDB // 4) ** -0.5, 0.25, ((0, 16),))
    residual = gaussian(key_list[10], (TOKENS, D), 1.0, 6.0, ((0, 512),))
    norm_gain = jnp.clip(1.0 + 0.18 * jax.random.normal(key_list[11], (D,), jnp.float32), 0.1, 1.9)
    expert_ids = draw_expert_ids(jax.random.fold_in(key_list[17], 71), 0)
    route_weight = jnp.clip(0.1 + 0.9 * jax.random.uniform(key_list[13], (TOKENS, TOP), jnp.float32) ** level_of(key_list[13], (TOKENS, TOP), ((0, 32),), -0.2, 0.2), 0.1, 1.0)
    gate_w = gaussian(key_list[14], (EXPERTS, D, DFF), D ** -0.5, 0.125, ((0, 32), (2, 16)))
    up_w = gaussian(key_list[15], (EXPERTS, D, DFF), D ** -0.5, 0.125, ((0, 32), (2, 16)))
    down_w = gaussian(key_list[16], (EXPERTS, DFF, D), DFF ** -0.5, 0.1875, ((0, 32), (2, 16)))
    return {"query_a": query_a, "key_a": key_a, "value_a": value_a, "cumlog_a": cumlog_a, "query_b": query_b, "key_b": key_b, "value_b": value_b, "cumlog_b": cumlog_b, "out_weight_a": out_weight_a, "out_weight_b": out_weight_b, "residual": residual, "norm_gain": norm_gain, "expert_ids": expert_ids, "route_weight": route_weight, "gate_w": gate_w, "up_w": up_w, "down_w": down_w}


norm_eps = 1e-05

def attend_group(queries, keys_in, values_in, gate_sums, heads, head_size):
    length = queries.shape[1]
    span = 256
    count_blocks = length // span
    query_heads = queries.reshape(heads, head_size, length)
    key_heads = keys_in.reshape(heads, head_size, length).astype(jnp.float32)
    value_heads = values_in.reshape(heads, head_size, length).astype(jnp.float32)
    positions = jnp.arange(length, dtype=jnp.int32)

    def one_block(index):
        offset = (index * span).astype(jnp.int32)
        query_block = lax.dynamic_slice_in_dim(query_heads, offset, span, 2).astype(jnp.float32)
        cum_block = lax.dynamic_slice_in_dim(gate_sums, offset, span, 1)
        scores = jnp.einsum('hdq,hdk->hqk', query_block, key_heads) * head_size ** (-0.5)
        scores = scores + cum_block[:, :, None] - gate_sums[:, None, :]
        rows_at = offset + jnp.arange(span, dtype=jnp.int32)
        scores = jnp.where(positions[None, None, :] <= rows_at[None, :, None], scores, -jnp.inf)
        weights = jax.nn.softmax(scores, axis=-1).astype(jnp.bfloat16)
        return jnp.einsum('hqk,hdk->hdq', weights.astype(jnp.float32), value_heads).astype(jnp.bfloat16)
    blocks = lax.map(one_block, jnp.arange(count_blocks, dtype=jnp.int32))
    return blocks.transpose(1, 2, 0, 3).reshape(heads * head_size, length)

def project_out(attn_a, attn_b, out_weight_a, out_weight_b):
    length = attn_a.shape[1]
    rows_a = attn_a.shape[0] // N_TP
    rows_b = attn_b.shape[0] // N_TP

    def add_part(total, index):
        part_a = lax.dynamic_slice_in_dim(attn_a, index * rows_a, rows_a, 0)
        part_b = lax.dynamic_slice_in_dim(attn_b, index * rows_b, rows_b, 0)
        weight_a = lax.dynamic_slice_in_dim(out_weight_a, index * rows_a, rows_a, 0)
        weight_b = lax.dynamic_slice_in_dim(out_weight_b, index * rows_b, rows_b, 0)
        term = jnp.dot(part_a.T, weight_a, preferred_element_type=jnp.float32)
        term = term + jnp.dot(part_b.T, weight_b, preferred_element_type=jnp.float32)
        rounded = lax.optimization_barrier(term.astype(jnp.bfloat16))
        return (total + rounded.astype(jnp.float32), None)
    total, _ = lax.scan(add_part, jnp.zeros((length, D), jnp.float32), jnp.arange(N_TP, dtype=jnp.int32))
    return total

def experts_out(normed, expert_ids, route_weight, gate_w, up_w, down_w):
    flat_ids = expert_ids.reshape(N_SP, TOK_DEV * TOP)
    marks = (flat_ids[:, :, None] == jnp.arange(EXPERTS, dtype=jnp.int32)[None, None, :]).astype(jnp.int32)
    before = jnp.cumsum(marks, axis=1) - marks
    rank = lax.optimization_barrier(jnp.sum(before * marks, axis=2))
    source = jnp.arange(N_SP, dtype=jnp.int32)[:, None]
    per_expert = N_SP * CAP
    where_to = (flat_ids * per_expert + source * CAP + rank).reshape(-1).astype(jnp.int32)
    token_of = jnp.repeat(jnp.arange(TOKENS, dtype=jnp.int32), TOP)
    table = jnp.zeros((EXPERTS * per_expert,), jnp.int32).at[where_to].set(token_of)
    filled = jnp.zeros((EXPERTS * per_expert,), jnp.float32).at[where_to].set(1.0)

    def one_expert(index):
        picks = lax.dynamic_slice_in_dim(table, index * per_expert, per_expert, 0)
        live = lax.dynamic_slice_in_dim(filled, index * per_expert, per_expert, 0)
        rows = normed[picks] * live[:, None].astype(normed.dtype)
        gate = jnp.dot(rows, gate_w[index], preferred_element_type=jnp.float32)
        upper = jnp.dot(rows, up_w[index], preferred_element_type=jnp.float32)
        hidden = (jax.nn.silu(gate) * upper).astype(jnp.bfloat16)
        return jnp.dot(hidden, down_w[index], preferred_element_type=jnp.float32).astype(jnp.bfloat16)
    results = lax.map(one_expert, jnp.arange(EXPERTS, dtype=jnp.int32))
    flat_out = results.reshape(EXPERTS * per_expert, D)
    chosen = flat_out[where_to].reshape(TOKENS, TOP, D).astype(jnp.float32)
    return lax.optimization_barrier(jnp.sum(chosen * route_weight[:, :, None], axis=1))

def reference(query_a, key_a, value_a, cumlog_a, query_b, key_b, value_b, cumlog_b, out_weight_a, out_weight_b, residual, norm_gain, expert_ids, route_weight, gate_w, up_w, down_w):
    attn_a = attend_group(query_a, key_a, value_a, cumlog_a, HA, HDA)
    attn_b = attend_group(query_b, key_b, value_b, cumlog_b, HB, HDB)
    mixed = project_out(attn_a, attn_b, out_weight_a, out_weight_b)
    summed = residual.astype(jnp.float32) + mixed
    center = summed - lax.optimization_barrier(jnp.mean(summed, axis=-1, keepdims=True))
    variance = lax.optimization_barrier(jnp.mean(center * center, axis=-1, keepdims=True))
    normed = (center * lax.rsqrt(variance + norm_eps) * norm_gain).astype(jnp.bfloat16)
    routed = experts_out(normed, expert_ids, route_weight, gate_w, up_w, down_w)
    return (normed.astype(jnp.float32) + routed).astype(jnp.bfloat16)
```

```python
import jax
import jax.numpy as jnp
from jax import lax
from jax.experimental import pallas as pl
from jax.experimental.pallas import tpu as pltpu
from jax.sharding import PartitionSpec as P

MESH = pl.DeviceIdType.MESH
F32 = jnp.float32
BF16 = jnp.bfloat16
HDA = 64
HDB = 128
NZ = 16
HALF = NZ // 2
LOG2E = 1.4426950408889634
NORM_EPS = 1e-05


def remote(src, dst, send_sem, recv_sem, device):
    return pltpu.make_async_remote_copy(
        src_ref=src, dst_ref=dst, send_sem=send_sem, recv_sem=recv_sem,
        device_id=device, device_id_type=MESH,
    )


def nt(a, b):
    return lax.dot_general(a, b, (((1,), (1,)), ((), ())), preferred_element_type=F32)


def nn(a, b):
    return lax.dot_general(a, b, (((1,), (0,)), ((), ())), preferred_element_type=F32)


def kernel(
    qa_ref, ka_ref, va_ref, cuma_ref, qb_ref, kb_ref, vb_ref, cumb_ref,
    woa_ref, wob_ref, res_ref, gain_ref, ids_ref, rw_ref, gate_ref, up_ref, down_ref,
    out_ref,
    kv, wall, dall, woa, wob, qta, qtb, top_a, top_b, sum_a, sum_b, acc_a, acc_b,
    pick, mix_hi, mix_lo, rs_send, rs_recv, n_send, n_recv, d_send, xr, xall,
    h_own, hall, o_send, ret,
    load_sem, kv_recv_p, kv_recv_m, kv_recv_s, kv_send_p, kv_send_m, kv_send_s,
    w_recv, w_send, rs_sems, n_sems, d_sems, x_recv, x_send, h_recv, h_send, o_sems,
):
    sp = lax.axis_index("sp")
    tp = lax.axis_index("tp")
    z, c = sp // 2, sp % 2
    y, x = tp // 4, tp % 4
    quarter = z % 4
    place = (z // 4) * 2 + c
    at_home = y == quarter
    up_z = (2 * ((z + 1) % NZ) + c, tp)
    down_z = (2 * ((z + NZ - 1) % NZ) + c, tp)
    sibling = (2 * z + 1 - c, tp)
    up_y = (sp, ((y + 1) % 4) * 4 + x)
    down_y = (sp, ((y + 3) % 4) * 4 + x)

    barrier = pltpu.get_barrier_semaphore()
    for device in (up_z, down_z, sibling):
        pl.semaphore_signal(barrier, inc=1, device_id=device, device_id_type=MESH)

    @pl.loop(1, 16)
    def _(r):
        pl.semaphore_signal(barrier, inc=1, device_id=(sp, (tp + r) % 16), device_id_type=MESH)

    @pl.loop(0, 32)
    def _(e):
        @pl.when(jnp.logical_or(e != sp, jnp.logical_not(at_home)))
        def _():
            pl.semaphore_signal(barrier, inc=1, device_id=(e, quarter * 4 + x), device_id_type=MESH)

        i, ys = e % 8, e // 8
        s = 2 * (y + 4 * (i // 2)) + i % 2

        @pl.when(jnp.logical_or(s != sp, ys != y))
        def _():
            pl.semaphore_signal(barrier, inc=1, device_id=(s, ys * 4 + x), device_id_type=MESH)

    own = kv.at[sp]
    kv_loads = [
        pltpu.make_async_copy(ka_ref, own.at[0, pl.ds(0, HDA)], load_sem.at[0]),
        pltpu.make_async_copy(va_ref, own.at[0, pl.ds(HDA, HDA)], load_sem.at[1]),
        pltpu.make_async_copy(kb_ref, own.at[1], load_sem.at[2]),
        pltpu.make_async_copy(vb_ref, own.at[2], load_sem.at[3]),
    ]
    w_loads = [
        pltpu.make_async_copy(gate_ref, wall.at[y, pl.ds(0, 64)], load_sem.at[4]),
        pltpu.make_async_copy(up_ref, wall.at[y, pl.ds(64, 64)], load_sem.at[5]),
    ]
    o_loads = [
        pltpu.make_async_copy(woa_ref, woa, load_sem.at[6]),
        pltpu.make_async_copy(wob_ref, wob, load_sem.at[7]),
    ]
    d_loads = [
        pltpu.make_async_copy(
            down_ref.at[pl.ds((4 * b + a) * 64, 64)],
            dall.at[y, pl.ds((4 * a + b) * 64, 64)],
            load_sem.at[8 + 4 * a + b],
        )
        for a in range(4)
        for b in range(4)
    ]
    for copy in kv_loads + w_loads + d_loads + o_loads:
        copy.start()

    expert_of = lax.broadcasted_iota(jnp.int32, (32, 128), 0)
    id0, id1 = ids_ref[0:1, :], ids_ref[1:2, :]
    marks = (expert_of == id0).astype(F32) + (expert_of == id1).astype(F32)
    before = lax.broadcasted_iota(jnp.int32, (128, 128), 0) < lax.broadcasted_iota(
        jnp.int32, (128, 128), 1
    )
    rank = nn(marks.astype(BF16), before.astype(F32).astype(BF16))
    spread = (
        lax.broadcasted_iota(jnp.int32, (512, 32), 0) // 16
        == lax.broadcasted_iota(jnp.int32, (512, 32), 1)
    ).astype(F32).astype(BF16)
    marks_at = nn(spread, marks.astype(BF16))
    rank_at = nn(spread, rank.astype(BF16))
    slot = lax.broadcasted_iota(jnp.int32, (512, 128), 0)
    chosen = jnp.logical_and(marks_at > 0.5, rank_at == (slot % 16).astype(F32))
    pick[...] = chosen.astype(F32).astype(BF16)
    weight = jnp.where(
        chosen, jnp.where(slot // 16 == id0, rw_ref[0:1, :], rw_ref[1:2, :]), 0.0
    )
    weight_t = weight.T
    high = weight_t.astype(BF16)
    mix_hi[...] = high
    mix_lo[...] = (weight_t - high.astype(F32)).astype(BF16)
    qta[...] = qa_ref[...].astype(F32).T.astype(BF16)
    qtb[...] = qb_ref[...].astype(F32).T.astype(BF16)
    for ref in (top_a, top_b):
        ref[...] = jnp.full(ref.shape, -jnp.inf, F32)
    for ref in (sum_a, sum_b, acc_a, acc_b):
        ref[...] = jnp.zeros(ref.shape, F32)

    for copy in kv_loads + w_loads + d_loads:
        copy.wait()
    at_home_count = jnp.where(at_home, 1, 0)
    pl.semaphore_wait(barrier, 18 + 2 * (32 - at_home_count))

    def send_p(k, j):
        src = 2 * (z - k + NZ) % (2 * NZ) + c
        return remote(kv.at[src, j], kv.at[src, j], kv_send_p.at[k, j], kv_recv_p.at[k, j], up_z)

    def recv_p(k, j):
        src = 2 * (z - k) + c
        return remote(
            kv.at[src, j], kv.at[src, j], kv_send_p.at[k, j], kv_recv_p.at[k - 1, j], up_z
        )

    def send_m(k, j):
        src = 2 * ((z + k) % NZ) + c
        return remote(kv.at[src, j], kv.at[src, j], kv_send_m.at[k, j], kv_recv_m.at[k, j], down_z)

    def recv_m(k, j):
        src = 2 * ((z + k) % NZ) + c
        return remote(
            kv.at[src, j], kv.at[src, j], kv_send_m.at[k, j], kv_recv_m.at[k - 1, j], down_z
        )

    def send_s(zz):
        src = 2 * zz + c
        return remote(kv.at[src], kv.at[src], kv_send_s.at[zz], kv_recv_s.at[zz], sibling)

    def recv_s(zz):
        src = 2 * zz + 1 - c
        return remote(kv.at[src], kv.at[src], kv_send_s.at[zz], kv_recv_s.at[zz], sibling)

    def valid_p(k):
        return z - k >= 0

    def go_p(k):
        return jnp.logical_and(z - k >= 0, z < NZ - 1)

    def valid_m(k):
        return (z + k) % NZ <= HALF - 2

    def useful_m(k):
        return z + k - NZ >= 0

    def fold(shards, masked):
        zs = [kv.at[s] for s in shards]
        keys_a = jnp.concatenate([s[0, 0:HDA] for s in zs], axis=1)
        vals_a = jnp.concatenate([s[0, HDA : 2 * HDA] for s in zs], axis=1)
        keys_b = jnp.concatenate([s[1] for s in zs], axis=1)
        vals_b = jnp.concatenate([s[2] for s in zs], axis=1)
        for keys, vals, qt, cum, top, total, acc, size in (
            (keys_a, vals_a, qta, cuma_ref, top_a, sum_a, acc_a, HDA),
            (keys_b, vals_b, qtb, cumb_ref, top_b, sum_b, acc_b, HDB),
        ):
            at = pl.multiple_of(sp * 128, 128)
            base = cum[0:1, pl.ds(at, 128)][0:1, 0:1]
            bias = jnp.concatenate(
                [
                    (base - cum[0:1, pl.ds(pl.multiple_of(s * 128, 128), 128)]) * LOG2E
                    for s in shards
                ],
                axis=1,
            )
            scores = nn(qt[...], keys) * (size**-0.5 * LOG2E) + bias
            if masked:
                hidden = lax.broadcasted_iota(jnp.int32, scores.shape, 1) > (
                    lax.broadcasted_iota(jnp.int32, scores.shape, 0)
                )
                scores = jnp.where(hidden, -jnp.inf, scores)
            old = top[:, 0:1]
            new = jnp.maximum(old, jnp.max(scores, axis=1, keepdims=True))
            keep = jnp.exp2(old - new)
            weights = jnp.exp2(scores - new)
            added = jnp.sum(weights, axis=1, keepdims=True)
            total[...] = total[...] * keep + added
            acc[...] = acc[...] * keep + nt(weights.astype(BF16), vals)
            top[...] = jnp.broadcast_to(new, top.shape)

    for j in range(3):
        @pl.when(z < NZ - 1)
        def _():
            send_p(0, j).start()

        @pl.when(z <= HALF - 2)
        def _():
            send_m(0, j).start()

    @pl.when(c == 0)
    def _():
        send_s(z).start()

    def part(v, half):
        return wall.at[v, pl.ds(64 * half, 64)] if half < 2 else dall.at[v, pl.ds(512 * (half - 2), 512)]

    def w_first(half, sign):
        index = half * 3 + (0 if sign > 0 else 1)
        device = up_y if sign > 0 else down_y
        return remote(part(y, half), part(y, half), w_send.at[index], w_recv.at[index], device)

    def w_got(half, sign):
        index = half * 3 + (0 if sign > 0 else 1)
        v = (y + 3) % 4 if sign > 0 else (y + 1) % 4
        return remote(part(v, half), part(v, half), w_send.at[index], w_recv.at[index], up_y)

    def w_relay(half):
        index = half * 3 + 2
        v, device = ((y + 3) % 4, up_y) if half % 2 == 0 else ((y + 1) % 4, down_y)
        return remote(part(v, half), part(v, half), w_send.at[index], w_recv.at[index], device)

    def w_got_relay(half):
        index = half * 3 + 2
        v = (y + 2) % 4
        return remote(part(v, half), part(v, half), w_send.at[index], w_recv.at[index], up_y)

    for half in (0, 1):
        w_first(half, 1 if half == 0 else -1).start()
    for half in (0, 1):
        w_first(half, -1 if half == 0 else 1).start()

    fold([sp], True)

    @pl.when(c == 1)
    def _():
        recv_s(z).wait_recv()
        fold([sp - 1], False)

    def use(zz):
        recv_s(zz).wait_recv()
        fold([2 * zz, 2 * zz + 1], False)

    @pl.loop(1, HALF + 1)
    def _(k):
        for j in range(3):
            @pl.when(valid_p(k))
            def _():
                recv_p(k, j).wait_recv()

            @pl.when(jnp.logical_and(go_p(k), k < HALF))
            def _():
                send_p(k, j).start()

            @pl.when(jnp.logical_and(valid_m(k), k < HALF))
            def _():
                recv_m(k, j).wait_recv()

            @pl.when(jnp.logical_and(valid_m(k), k < HALF - 1))
            def _():
                send_m(k, j).start()

        @pl.when(valid_p(k))
        def _():
            send_s(z - k).start()

        @pl.when(jnp.logical_and(useful_m(k), k < HALF))
        def _():
            send_s(z + k - NZ).start()

        @pl.when(jnp.logical_and(valid_p(k - 1), k > 1))
        def _():
            use(z - k + 1)

        @pl.when(jnp.logical_and(useful_m(k - 1), k > 1))
        def _():
            use(z + k - 1 - NZ)

        @pl.when(k == 4)
        def _():
            w_got(0, 1).wait_recv()
            w_relay(0).start()
            w_got(1, -1).wait_recv()
            w_relay(1).start()
            w_first(2, 1).start()
            w_first(3, -1).start()
            w_first(2, -1).start()
            w_first(3, 1).start()

    @pl.when(valid_p(HALF))
    def _():
        use(z - HALF)

    for copy in o_loads:
        copy.wait()
    attn_a = (acc_a[...] / sum_a[...]).astype(BF16)
    attn_b = (acc_b[...] / sum_b[...]).astype(BF16)
    for n in range(4):
        cols = pl.ds(512 * n, 512)
        term = nn(attn_a, woa[:, cols]) + nn(attn_b, wob[:, cols])
        rs_send[:, :, cols] = term.reshape(16, 8, 512).astype(BF16)

    @pl.loop(1, 16)
    def _(r):
        p = (tp + r) % 16
        remote(rs_send.at[p], rs_recv.at[r - 1], rs_sems.at[0], rs_sems.at[1], (sp, p)).start()

    mixed = rs_send[tp].astype(F32)
    remote(rs_recv, rs_recv, rs_sems.at[0], rs_sems.at[1], up_y).wait_recv()
    for r in range(15):
        mixed = mixed + rs_recv[r].astype(F32)
    summed = res_ref[...].astype(F32) + mixed
    center = summed - jnp.mean(summed, axis=1, keepdims=True)
    variance = jnp.mean(center * center, axis=1, keepdims=True)
    normed_rows = (center * lax.rsqrt(variance + NORM_EPS) * gain_ref[...]).astype(BF16).astype(F32)
    for j in range(16):
        n_send[j] = normed_rows[:, 128 * j : 128 * (j + 1)]
    n_recv[tp] = n_send[tp]

    @pl.loop(1, 16)
    def _(r):
        p = (tp + r) % 16
        remote(n_send.at[p], n_recv.at[tp], n_sems.at[0], n_sems.at[1], (sp, p)).start()

    most = pl.ds(0, 15)
    remote(n_send.at[most], n_recv.at[most], n_sems.at[0], n_sems.at[1], up_y).wait_recv()
    normed = n_recv[...].reshape(128, 128)

    d_send[...] = nn(pick[...], normed.astype(BF16)).astype(BF16).reshape(32, 16, 128)

    @pl.loop(0, 32)
    def _(e):
        @pl.when(jnp.logical_or(e != sp, jnp.logical_not(at_home)))
        def _():
            remote(
                d_send.at[e], xr.at[y * 8 + place], d_sems.at[0], d_sems.at[1],
                (e, quarter * 4 + x),
            ).start()

    w_got(2, 1).wait_recv()
    w_relay(2).start()
    w_got(3, -1).wait_recv()
    w_relay(3).start()

    @pl.when(at_home)
    def _():
        xr[y * 8 + place] = d_send[sp]

    def wait_32(ref, sems):
        for count, flag in ((31, at_home), (32, jnp.logical_not(at_home))):
            @pl.when(flag)
            def _():
                view = ref.at[pl.ds(0, count)]
                remote(view, view, sems.at[0], sems.at[1], up_y).wait_recv()

    wait_32(xr, d_sems)
    for r in range(1, 4):
        remote(
            xr, xall.at[r - 1], x_send.at[r - 1], x_recv.at[r - 1], (sp, y * 4 + (x + r) % 4)
        ).start()

    w_got(0, -1).wait_recv()
    w_got(1, 1).wait_recv()
    w_got_relay(0).wait_recv()
    w_got_relay(1).wait_recv()

    def gate_up(ref, xx):
        lhs, gates, ups = [], [], []
        for ys in range(4):
            lhs.append(ref[8 * ys : 8 * ys + 8].reshape(128, 128))
            cols = pl.ds(pl.multiple_of((4 * ys + xx) * 128, 128), 128)
            gates.append(wall[:, 0:64, cols].reshape(256, 128))
            ups.append(wall[:, 64:128, cols].reshape(256, 128))
        lhs = jnp.concatenate(lhs, axis=1)
        return nt(lhs, jnp.concatenate(gates, axis=1)), nt(lhs, jnp.concatenate(ups, axis=1))

    gate, upper = gate_up(xr, x)
    for r in (1, 3, 2):
        remote(
            xr, xall.at[r - 1], x_send.at[r - 1], x_recv.at[r - 1], up_y
        ).wait_recv()
        more_gate, more_up = gate_up(xall.at[r - 1], (x + 4 - r) % 4)
        gate, upper = gate + more_gate, upper + more_up
    h_own[...] = (gate / (1.0 + jnp.exp(-gate)) * upper).astype(BF16)
    for r in range(1, 4):
        remote(
            h_own, hall.at[r - 1], h_send.at[r - 1], h_recv.at[r - 1], (sp, y * 4 + (x + r) % 4)
        ).start()

    w_got(2, -1).wait_recv()
    w_got(3, 1).wait_recv()
    w_got_relay(2).wait_recv()
    w_got_relay(3).wait_recv()

    def downward(hidden, xx):
        rows = pl.ds(pl.multiple_of(xx * 256, 256), 256)
        return nn(hidden, jnp.concatenate([dall[v, rows, :] for v in range(4)], axis=1))

    result = downward(h_own[...], x)
    for r in (1, 3, 2):
        remote(
            h_own, hall.at[r - 1], h_send.at[r - 1], h_recv.at[r - 1], up_y
        ).wait_recv()
        result = result + downward(hall[r - 1], (x + 4 - r) % 4)
    for v in range(4):
        o_send[8 * v : 8 * v + 8] = (
            result[:, 128 * v : 128 * (v + 1)].astype(BF16).reshape(8, 16, 128)
        )

    @pl.loop(0, 32)
    def _(n):
        i, v = n % 8, n // 8
        s = 2 * (y + 4 * (i // 2)) + i % 2

        @pl.when(jnp.logical_or(s != sp, v != y))
        def _():
            remote(
                o_send.at[n], ret.at[sp], o_sems.at[0], o_sems.at[1], (s, v * 4 + x)
            ).start()

    @pl.when(at_home)
    def _():
        ret[sp] = o_send[y * 8 + place]

    wait_32(ret, o_sems)
    back = ret[...].reshape(512, 128)
    routed = nn(mix_hi[...], back) + nn(mix_lo[...], back)
    out_ref[...] = (normed + routed).astype(BF16)

    for j in range(3):
        @pl.when(z < NZ - 1)
        def _():
            send_p(0, j).wait_send()

        @pl.when(z <= HALF - 2)
        def _():
            send_m(0, j).wait_send()

    @pl.when(c == 0)
    def _():
        send_s(z).wait_send()

    @pl.loop(1, HALF + 1)
    def _(k):
        for j in range(3):
            @pl.when(jnp.logical_and(go_p(k), k < HALF))
            def _():
                send_p(k, j).wait_send()

            @pl.when(jnp.logical_and(valid_m(k), k < HALF - 1))
            def _():
                send_m(k, j).wait_send()

        @pl.when(valid_p(k))
        def _():
            send_s(z - k).wait_send()

        @pl.when(jnp.logical_and(useful_m(k), k < HALF))
        def _():
            send_s(z + k - NZ).wait_send()

    for half in range(4):
        w_first(half, 1).wait_send()
        w_first(half, -1).wait_send()
        w_relay(half).wait_send()
    remote(rs_recv, rs_recv, rs_sems.at[0], rs_sems.at[1], up_y).wait_send()
    remote(n_send.at[most], n_recv.at[most], n_sems.at[0], n_sems.at[1], up_y).wait_send()
    for r in range(1, 4):
        remote(xr, xall.at[r - 1], x_send.at[r - 1], x_recv.at[r - 1], up_y).wait_send()
        remote(h_own, hall.at[r - 1], h_send.at[r - 1], h_recv.at[r - 1], up_y).wait_send()
    for ref, sems in ((d_send, d_sems), (o_send, o_sems)):
        for count, flag in ((31, at_home), (32, jnp.logical_not(at_home))):
            @pl.when(flag)
            def _():
                view = ref.at[pl.ds(0, count)]
                remote(view, view, sems.at[0], sems.at[1], up_y).wait_send()


def per_device(
    query_a, key_a, value_a, cumlog_a, query_b, key_b, value_b, cumlog_b,
    out_weight_a, out_weight_b, residual, norm_gain, expert_ids, route_weight,
    gate_w, up_w, down_w,
):
    vm = pl.BlockSpec(memory_space=pltpu.VMEM)
    hbm = pl.BlockSpec(memory_space=pl.ANY)
    dma = pltpu.SemaphoreType.DMA
    return pl.pallas_call(
        kernel,
        out_shape=jax.ShapeDtypeStruct((128, 128), BF16),
        in_specs=[
            vm, hbm, hbm, vm, vm, hbm, hbm, vm, hbm, hbm, vm, vm, vm, vm, hbm, hbm, hbm,
        ],
        out_specs=vm,
        scratch_shapes=[
            pltpu.VMEM((32, 3, 128, 128), BF16),
            pltpu.VMEM((4, 128, 2048), BF16),
            pltpu.VMEM((4, 1024, 128), BF16),
            pltpu.VMEM((64, 2048), BF16),
            pltpu.VMEM((128, 2048), BF16),
            pltpu.VMEM((128, 64), BF16),
            pltpu.VMEM((128, 128), BF16),
            pltpu.VMEM((128, 128), F32),
            pltpu.VMEM((128, 128), F32),
            pltpu.VMEM((128, 64), F32),
            pltpu.VMEM((128, 128), F32),
            pltpu.VMEM((128, 64), F32),
            pltpu.VMEM((128, 128), F32),
            pltpu.VMEM((512, 128), BF16),
            pltpu.VMEM((128, 512), BF16),
            pltpu.VMEM((128, 512), BF16),
            pltpu.VMEM((16, 8, 2048), BF16),
            pltpu.VMEM((15, 8, 2048), BF16),
            pltpu.VMEM((16, 8, 128), F32),
            pltpu.VMEM((16, 8, 128), F32),
            pltpu.VMEM((32, 16, 128), BF16),
            pltpu.VMEM((32, 16, 128), BF16),
            pltpu.VMEM((3, 32, 16, 128), BF16),
            pltpu.VMEM((128, 256), BF16),
            pltpu.VMEM((3, 128, 256), BF16),
            pltpu.VMEM((32, 16, 128), BF16),
            pltpu.VMEM((32, 16, 128), BF16),
            dma((24,)),
            dma((HALF, 3)),
            dma((HALF, 3)),
            dma((NZ,)),
            dma((HALF, 3)),
            dma((HALF, 3)),
            dma((NZ,)),
            dma((12,)),
            dma((12,)),
            dma((2,)),
            dma((2,)),
            dma((2,)),
            dma((3,)),
            dma((3,)),
            dma((3,)),
            dma((3,)),
            dma((2,)),
        ],
        compiler_params=pltpu.CompilerParams(
            collective_id=0, has_side_effects=True, vmem_limit_bytes=48 * 1024 * 1024
        ),
        name="layer",
    )(
        query_a, key_a, value_a, cumlog_a, query_b, key_b, value_b, cumlog_b,
        out_weight_a, out_weight_b, residual, norm_gain.reshape(1, -1),
        expert_ids.T, route_weight.T, gate_w[0].T, up_w[0].T, down_w[0],
    )


def solution(mesh):
    placed = (
        P("tp", "sp"), P("tp", "sp"), P("tp", "sp"), P("tp", None),
        P("tp", "sp"), P("tp", "sp"), P("tp", "sp"), P("tp", None),
        P("tp", None), P("tp", None), P(("sp", "tp"), None), P(),
        P("sp", None), P("sp", None),
        P("sp", None, "tp"), P("sp", None, "tp"), P("sp", None, "tp"),
    )
    return jax.shard_map(
        per_device, mesh=mesh, in_specs=placed, out_specs=P("sp", "tp"), check_vma=False
    )
```
